512 devices in a mesh: fs: 16 (over y, x), tp: 32 (over z, core).
Axes of the slice: x: 4, y: 4, z: 16, core: 2. Of those that a mesh axis runs over, the one named last changes fastest.
Arguments:
- tokens: bfloat16 [16384, 2048], P(('fs', 'tp')), may hold values from -6 to 6
- norm_gain: float32 [2048], P('fs'), may hold values from 0.1 to 1.9
- gate_master: float32 [2048, 8192], P('fs', 'tp'), may hold values from -0.125 to 0.125
- up_master: float32 [2048, 8192], P('fs', 'tp'), may hold values from -0.125 to 0.125
- down_master: float32 [2048, 8192], P('fs', 'tp'), may hold values from -0.125 to 0.125
Outputs:
- mixed: bfloat16 [16384, 2048], P(('fs', 'tp'))
- gate_ready: bfloat16 [2048, 8192], P(None, 'tp')
- up_ready: bfloat16 [2048, 8192], P(None, 'tp')
- down_ready: bfloat16 [2048, 8192], P(None, 'tp')
The draws below stay inside these ranges and needn't reach their ends.
All inputs are finite; a program needn't handle non-finite values.
Results may differ from the reference program's by a relative error of at most 0.0095.
Values may be sent and summed in bfloat16 or wider, within the bound.
A program may use at most 64 MiB of HBM per device.

```python
import jax
import jax.numpy as jnp
from jax import lax

D = 2048
FF = 8192
TOKENS = 16384
N_TP = 32


def spiked(drawn, stream_key, source, target, blocks, factor):
    owner, partner = [(jnp.arange(drawn.shape[position]) // (drawn.shape[position] // blocks)).reshape([-1 if axis == position else 1 for axis in range(drawn.ndim)]) for position in (source, target)]
    chosen = jax.random.permutation(stream_key, blocks)[partner]
    strong = (owner == chosen) | (owner == (partner + blocks // 2) % blocks)
    return jnp.where(strong, factor * drawn, drawn)


def level_of(rng, shape, shards, low, high):
    loudness, own = 1.0, jax.random.fold_in(rng, 6)
    for dim, shards_of in shards:
        heights = jnp.exp(jax.random.uniform(jax.random.fold_in(own, dim), (shards_of,), jnp.float32, low / len(shards), high / len(shards)))
        loudness = loudness * jnp.repeat(heights, shape[dim] // shards_of).reshape([-1 if axis == dim else 1 for axis in range(len(shape))])
    return loudness


def centred(key, dims, spread, limit, cuts=(), dtype=jnp.bfloat16):
    drawn = spread * jax.random.normal(key, dims, jnp.float32)
    if cuts:
        drawn = drawn * level_of(key, dims, cuts, -0.22, 0.18)
    return jnp.clip(drawn, -limit, limit).astype(dtype)


def heavy_noise(key, dims, deviation, bound, split, heavy, held_as=jnp.bfloat16):
    drawn = deviation * jax.random.normal(key, dims, jnp.float32)
    if split:
        drawn = drawn * level_of(key, dims, split, -0.22, 0.18)
    return jnp.clip(spiked(drawn, jax.random.fold_in(key, 3), *heavy), -bound, bound).astype(held_as)


def setup_inputs(seed: int = 0) -> dict:
    key_of = jax.random.split(jax.random.key(seed), 6)
    tokens = centred(key_of[0], (TOKENS, D), 1.0, 6.0, ((0, 512),))
    norm_gain = jnp.clip(1.0 + 0.18 * jax.random.normal(key_of[1], (D,), jnp.float32), 0.1, 1.9)
    gate_master = centred(key_of[2], (D, FF), D ** -0.5, 0.125, ((0, 16), (1, 32)), jnp.float32)
    up_master = centred(key_of[3], (D, FF), D ** -0.5, 0.125, ((0, 16), (1, 32)), jnp.float32)
    down_master = heavy_noise(key_of[4], (D, FF), FF ** -0.5, 0.125, ((0, 16), (1, 32)), (1, 0, 32, 2.75), jnp.float32)
    return {"tokens": tokens, "norm_gain": norm_gain, "gate_master": gate_master, "up_master": up_master, "down_master": down_master}


def reference(tokens, norm_gain, gate_master, up_master, down_master):
    gate_ready = (norm_gain[:, None] * gate_master).astype(jnp.bfloat16)
    up_ready = (norm_gain[:, None] * up_master).astype(jnp.bfloat16)
    down_ready = down_master.astype(jnp.bfloat16)
    tokens_wide = tokens.astype(jnp.float32)
    row_scale = lax.rsqrt(lax.optimization_barrier(jnp.mean(tokens_wide * tokens_wide, axis=1, keepdims=True)) + 1e-06)
    gate_proj = row_scale * jnp.dot(tokens, gate_ready, preferred_element_type=jnp.float32)
    up_proj = row_scale * jnp.dot(tokens, up_ready, preferred_element_type=jnp.float32)
    hidden = (jax.nn.silu(gate_proj) * up_proj).astype(jnp.bfloat16)
    block_width = FF // N_TP
    summed = jnp.zeros((tokens.shape[0], tokens.shape[1]), jnp.float32)
    for column_block in range(N_TP):
        lower = column_block * block_width
        partial_value = lax.dot_general(hidden[:, lower:lower + block_width], down_ready[:, lower:lower + block_width], (((1,), (1,)), ((), ())), preferred_element_type=jnp.float32)
        summed = summed + lax.optimization_barrier(partial_value.astype(jnp.bfloat16)).astype(jnp.float32)
    mixed = (tokens_wide + 0.5 * summed).astype(jnp.bfloat16)
    return (mixed, gate_ready, up_ready, down_ready)
```

```python
import jax
import jax.numpy as jnp
from jax import lax
from jax.experimental import pallas as pl
from jax.experimental.pallas import tpu as pltpu
from jax.sharding import Mesh
from jax.sharding import PartitionSpec as P

AXES = ("y", "x", "z", "c")
NZ = 16
NR = 4
HOPS = NZ // 2
NC = 8
CW = 256
ROWS = 32
D = 2048
W_DELAY = 8
MESH = pl.DeviceIdType.MESH


def kernel(tok, gain, gate_m, up_m, down_m, mixed, gate_o, up_o, down_o,
           T, W, M, G, H, PS, RV, SD, O,
           load_sem, tok_sem, ag_s, ag_r, rs_s, rs_r, xy_s, xy_r, dd_s, dd_r, out_sem):
    y, x, z, c = (lax.axis_index(a) for a in AXES)
    zto = ({"z": (z + 1) % NZ}, {"z": (z + NZ - 1) % NZ})
    f = 1 - 2 * c
    here = (x, y)
    names = ("x", "y")

    tok_loads = [pltpu.make_async_copy(tok.at[:, pl.ds(q * CW, CW)], T.at[z, q], tok_sem) for q in range(NC)]
    for copy in tok_loads:
        copy.start()
    gain_load = pltpu.make_async_copy(gain, G, load_sem.at[0])
    gain_load.start()
    m_loads = [pltpu.make_async_copy(src, M.at[j], load_sem.at[1 + j]) for j, src in enumerate((gate_m, up_m, down_m))]
    for copy in m_loads:
        copy.start()

    barrier = pltpu.get_barrier_semaphore()
    peers = [zto[0], zto[1], {"c": 1 - c}]
    for a in range(2):
        peers += [{names[a]: (here[a] + 1) % NR}, {names[a]: (here[a] + NR - 1) % NR}]
    for peer in peers:
        pl.semaphore_signal(barrier, inc=1, device_id=peer, device_id_type=MESH)

    own = y * NR + x
    gain_load.wait()
    g = jnp.broadcast_to(G[...], (128, 128)).T
    g = jnp.concatenate([g, g], axis=1)
    for j in range(3):
        m_loads[j].wait()
        value = M[j] * g if j < 2 else M[j]
        W[c, j, own] = value.astype(jnp.bfloat16).reshape(2, 64, 256)

    pltpu.make_async_copy(T.at[z], T.at[z], tok_sem).wait()
    pl.semaphore_wait(barrier, len(peers))

    def token_copy(way, step, q):
        block = (z + NZ - (step - 1)) % NZ if way == 0 else (z + step - 1) % NZ
        return pltpu.make_async_remote_copy(
            src_ref=T.at[block, q], dst_ref=T.at[block, q],
            send_sem=ag_s.at[way, 1 if step == HOPS else 0], recv_sem=ag_r.at[way, step - 1, q],
            device_id=zto[way], device_id_type=MESH)

    def token_wait(way, step, q):
        block = (z + NZ - step) % NZ if way == 0 else (z + step) % NZ
        pltpu.make_async_remote_copy(
            src_ref=T.at[block, q], dst_ref=T.at[block, q],
            send_sem=ag_s.at[way, 0], recv_sem=ag_r.at[way, step - 1, q],
            device_id=zto[way], device_id_type=MESH).wait_recv()

    def goes(way, q):
        return q < NC // 2 if way == 0 else q >= NC // 2

    def order(way, j):
        return j if way == 0 else (j + NC // 2) % NC

    for j in range(NC):
        for way in range(2):
            token_copy(way, 1, order(way, j)).start()

    def piece(h, r1, r2):
        a1 = here[h] + r1
        a2 = here[1 - h] + r2
        a1, a2 = (a1 + 2 * NR) % NR, (a2 + 2 * NR) % NR
        i = a2 * NR + a1 if h == 0 else a1 * NR + a2
        return W.at[c, :, i, h]

    off = (0, -f, f, 2)

    def weight_copy(h, ref, axis, sign, event):
        a = h if axis == 0 else 1 - h
        return pltpu.make_async_remote_copy(
            src_ref=ref, dst_ref=ref, send_sem=xy_s, recv_sem=xy_r.at[h * 15 + event],
            device_id={names[a]: (here[a] + sign * f + NR) % NR}, device_id_type=MESH)

    def sibling_copy(ref):
        return pltpu.make_async_remote_copy(
            src_ref=ref, dst_ref=ref, send_sem=dd_s, recv_sem=dd_r,
            device_id={"c": 1 - c}, device_id_type=MESH)

    for h in range(2):
        mine = piece(h, 0, 0)
        weight_copy(h, mine, 0, 1, 0).start()
        weight_copy(h, mine, 0, -1, 1).start()
    for h in range(2):
        mine = piece(h, 0, 0)
        weight_copy(h, mine, 1, 1, 3).start()
        weight_copy(h, mine, 1, -1, 7).start()
        sibling_copy(mine).start()

    def weight_event(h, event):
        if event < 3:
            r = event + 1
            ref = piece(h, off[r], 0)
        else:
            kind, r = divmod(event - 3, 4)
            ref = piece(h, off[r], (-f, f, 2)[kind])
        weight_copy(h, ref, 0, 1, event).wait_recv()
        if event == 0:
            weight_copy(h, ref, 0, 1, 2).start()
        if event < 3:
            weight_copy(h, ref, 1, 1, 3 + r).start()
            weight_copy(h, ref, 1, -1, 7 + r).start()
        elif event < 7:
            weight_copy(h, ref, 1, 1, 11 + r).start()
        sibling_copy(ref).start()

    weight_order = [(h, e) for e in (0, 1, 3, 7, 2, 4, 8, 5, 9, 11, 6, 10, 12, 13, 14) for h in range(2)]

    done = 0
    for step in range(1, HOPS + 1):
        for j in range(NC if step < HOPS else NC // 2):
            for way in range(2):
                q = order(way, j)
                token_wait(way, step, q)
                if step + 1 < HOPS or (step + 1 == HOPS and goes(way, q)):
                    token_copy(way, step + 1, q).start()
            due = ((step - 1) * NC + j - W_DELAY) * 5 // NC
            while done < min(due, 30):
                weight_event(*weight_order[done])
                done += 1
    while done < 30:
        weight_event(*weight_order[done])
        done += 1

    outs = [pltpu.make_async_copy(W.at[c, j], o, out_sem.at[j]) for j, o in enumerate((gate_o, up_o, down_o))]
    for copy in outs:
        copy.start()
    theirs = W.at[1 - c]
    pltpu.make_async_remote_copy(
        src_ref=theirs, dst_ref=theirs, send_sem=dd_s, recv_sem=dd_r,
        device_id={"c": 1 - c}, device_id_type=MESH).wait_recv()

    def expand(m, carry):
        parts = [T[pl.ds(m * 8, 8), q].reshape(256, CW) for q in range(NC)]
        total = jnp.zeros((256, 1), jnp.float32)
        for part in parts:
            wide = part.astype(jnp.float32)
            total = total + jnp.sum(wide * wide, axis=1, keepdims=True)
        scale = lax.rsqrt(total * (1.0 / D) + 1e-06)
        rows = jnp.concatenate(parts, axis=1)
        for k in range(2):
            gate = scale * jnp.dot(rows, W[k, 0].reshape(D, 256), preferred_element_type=jnp.float32)
            up = scale * jnp.dot(rows, W[k, 1].reshape(D, 256), preferred_element_type=jnp.float32)
            hid = gate / (1.0 + jnp.exp(-gate)) * up
            H[pl.ds(pl.multiple_of(m * 256, 256), 256), k * 256 : (k + 1) * 256] = hid.astype(jnp.bfloat16)
        return carry

    lax.fori_loop(0, 2, expand, 0)

    def dest(way, step):
        return (z + HOPS - step) % NZ if way == 0 else (z + HOPS + step) % NZ

    def sum_copy(way, step, q):
        return pltpu.make_async_remote_copy(
            src_ref=SD.at[way, step, q], dst_ref=RV.at[way, step, q],
            send_sem=rs_s.at[way, 1 if step == 0 else 0], recv_sem=rs_r.at[way, step, q],
            device_id=zto[way], device_id_type=MESH)

    for q in range(NC):
        value = None
        for k in range(2):
            part = lax.dot_general(H[:, k * 256 : (k + 1) * 256], W[k, 2, 2 * q : 2 * q + 2].reshape(256, 256),
                                   (((1,), (1,)), ((), ())), preferred_element_type=jnp.float32)
            value = part if value is None else value + part
        PS[:, q] = value.reshape(NZ, ROWS, CW)
        first = 0 if goes(0, q) else 1
        for way, step in ((first, 0), (1 - first, 1)):
            SD[way, step, q] = PS[dest(way, step), q].astype(jnp.bfloat16)
        for way, step in ((first, 0), (1 - first, 1)):
            sum_copy(way, step, q).start()

    for step in range(1, HOPS):
        for j in range(NC if step > 1 else NC // 2):
            for way in range(2):
                q = order(way, j) if step == 1 else order(1 - way, j)
                sum_copy(way, step - 1, q).wait_recv()
                SD[way, step, q] = (PS[dest(way, step), q] + RV[way, step - 1, q].astype(jnp.float32)).astype(jnp.bfloat16)
                sum_copy(way, step, q).start()

    last = []
    for q in range(NC):
        total = PS[z, q]
        for way in range(2):
            sum_copy(way, HOPS - 1, q).wait_recv()
            total = total + RV[way, HOPS - 1, q].astype(jnp.float32)
        O[:, q * CW : (q + 1) * CW] = (T[z, q].astype(jnp.float32) + 0.5 * total).astype(jnp.bfloat16)
    last = pltpu.make_async_copy(O, mixed, out_sem.at[3])
    last.start()

    def sent(ref, sem):
        pltpu.make_async_copy(ref, ref, sem).wait()

    for way in range(2):
        sent(T.at[pl.ds(0, HOPS - 1)], ag_s.at[way, 0])
        sent(T.at[0, pl.ds(0, NC // 2)], ag_s.at[way, 1])
        sent(T.at[pl.ds(0, HOPS - 1)], rs_s.at[way, 0])
        sent(T.at[0, pl.ds(0, NC // 2)], rs_s.at[way, 1])
    sent(W.at[0, :, pl.ds(0, 15)], xy_s)
    sent(W.at[0], dd_s)
    for copy in outs:
        copy.wait()
    last.wait()


def body(tokens, norm_gain, gate_master, up_master, down_master):
    ready = jax.ShapeDtypeStruct((16, 2, 64, 256), jnp.bfloat16)
    whole = pl.BlockSpec(memory_space=pl.ANY)
    dma = pltpu.SemaphoreType.DMA
    mixed, gate, up, down = pl.pallas_call(
        kernel,
        out_shape=(jax.ShapeDtypeStruct((ROWS, D), jnp.bfloat16), ready, ready, ready),
        in_specs=[whole] * 5,
        out_specs=(whole,) * 4,
        scratch_shapes=[
            pltpu.VMEM((NZ, NC, ROWS, CW), jnp.bfloat16),
            pltpu.VMEM((2, 3, 16, 2, 64, 256), jnp.bfloat16),
            pltpu.VMEM((3, 128, 256), jnp.float32),
            pltpu.VMEM((1, 128), jnp.float32),
            pltpu.VMEM((NZ * ROWS, 512), jnp.bfloat16),
            pltpu.VMEM((NZ, NC, ROWS, CW), jnp.float32),
            pltpu.VMEM((2, HOPS, NC, ROWS, CW), jnp.bfloat16),
            pltpu.VMEM((2, HOPS, NC, ROWS, CW), jnp.bfloat16),
            pltpu.VMEM((ROWS, D), jnp.bfloat16),
            dma((4,)),
            dma,
            dma((2, 2)),
            dma((2, HOPS, NC)),
            dma((2, 2)),
            dma((2, HOPS, NC)),
            dma,
            dma((30,)),
            dma,
            dma,
            dma((4,)),
        ],
        compiler_params=pltpu.CompilerParams(collective_id=0, has_side_effects=True, vmem_limit_bytes=50 * 2**20),
    )(tokens, norm_gain.reshape(1, 128), gate_master, up_master, down_master)
    return mixed, gate.reshape(D, 256), up.reshape(D, 256), down.reshape(D, 256)


def solution(mesh):
    split = Mesh(mesh.devices.reshape(NR, NR, NZ, 2), AXES)
    fs, tp = ("y", "x"), ("z", "c")
    return jax.shard_map(
        body,
        mesh=split,
        in_specs=(P(fs + tp, None), P(fs), P(fs, tp), P(fs, tp), P(fs, tp)),
        out_specs=(P(fs + tp, None), P(None, tp), P(None, tp), P(None, tp)),
        check_vma=False,
    )
```
